32 devices in a mesh: sp: 16 (over z, y, x), tp: 2 (over core).
Axes of the slice: x: 2, y: 2, z: 4, core: 2. Of those that a mesh axis runs over, the one named last changes fastest.
Arguments:
- queries: bfloat16 [8192, 8, 128], P('sp', 'tp'), may hold values from -60 to 60
- keys: bfloat16 [8192, 8, 128], P('sp', 'tp'), may hold values from -40 to 40
- values: bfloat16 [8192, 8, 128], P('sp', 'tp'), may hold values from -6 to 6
- w_out: bfloat16 [1024, 2048], P(None, 'tp'), may hold values from -0.1875 to 0.1875
Outputs:
- mixed: bfloat16 [8192, 2048], P('sp', 'tp')
The draws below stay inside these ranges and needn't reach their ends.
All inputs are finite; a program needn't handle non-finite values.
Results may differ from the reference program's by a relative error of at most 0.0051.
Values may be sent and summed in bfloat16 or wider, within the bound.
A program may use at most 64 MiB of HBM per device.

```python
import math
import jax
import jax.numpy as jnp
from jax import lax

D = 2048
HEADS = 8
HEAD_DIM = 128
W1 = 128
WINDOW_TWO = 512
DILATION_TWO = 4
WINDOW_THREE = 2048
DILATION_THREE = 16
TOKENS = 8192


def drawn_pair(key):
    shape = (TOKENS, HEADS, HEAD_DIM)
    starting_keys = jax.random.normal(jax.random.fold_in(key, 11), shape, jnp.float32)
    base_queries = jax.random.normal(jax.random.fold_in(key, 12), shape, jnp.float32) * 2.5
    return (jnp.clip(base_queries, -60.0, 60.0), jnp.clip(starting_keys, -40.0, 40.0))


def draw_queries(key, part):
    return drawn_pair(key)[0].astype(jnp.bfloat16)


def draw_keys(key, part):
    return drawn_pair(key)[1].astype(jnp.bfloat16)


def shard_levels(stream_key, dims, split, low, largest):
    def one(position, parts):
        draws = jax.random.uniform(jax.random.fold_in(jax.random.fold_in(stream_key, 6), position), (parts,), jnp.float32, low / len(split), largest / len(split))
        return jnp.repeat(jnp.exp(draws), dims[position] // parts).reshape((-1,) + (1,) * (len(dims) - position - 1))

    gain = one(*split[0])
    for cut in split[1:]:
        gain = gain * one(*cut)
    return gain


def gaussian(stream_key, extent, deviation, bound, shards=(), kind=jnp.bfloat16):
    values = deviation * jax.random.normal(stream_key, extent, jnp.float32)
    if shards:
        values = values * shard_levels(stream_key, extent, shards, -0.22, 0.18)
    return jnp.clip(values, -bound, bound).astype(kind)


def setup_inputs(seed: int = 0) -> dict:
    key_of = jax.random.split(jax.random.key(seed), 5)
    queries = draw_queries(jax.random.fold_in(key_of[4], 71), 0)
    keys = draw_keys(jax.random.fold_in(key_of[4], 71), 0)
    values = gaussian(key_of[2], (TOKENS, HEADS, HEAD_DIM), 1.0, 6.0, ((0, 16), (1, 2)))
    w_out = gaussian(key_of[3], (HEADS * HEAD_DIM, D), (HEADS * HEAD_DIM) ** -0.5, 0.1875, ((1, 2),))
    return dict(queries=queries, keys=keys, values=values, w_out=w_out)


def with_previous(blocks):
    earlier = jnp.concatenate([jnp.zeros_like(blocks[:1]), blocks[:-1]], axis=0)
    return jnp.concatenate([earlier, blocks], axis=1)

def single_branch(head_queries, head_keys, head_values, window, dilation):
    band_rows = window // dilation
    block_count = TOKENS // window
    shape = (block_count, band_rows, dilation, HEAD_DIM)
    query_blocks = head_queries.astype(jnp.float32).reshape(shape)
    key_bands = with_previous(head_keys.astype(jnp.float32).reshape(shape))
    value_bands = with_previous(head_values.astype(jnp.float32).reshape(shape))
    scores = jnp.einsum('nqrd,nkrd->nrqk', query_blocks, key_bands) / math.sqrt(HEAD_DIM)
    query_idx = jnp.arange(band_rows, dtype=jnp.int32)[:, None]
    key_idx = jnp.arange(2 * band_rows, dtype=jnp.int32)[None, :]
    distance = query_idx - key_idx + band_rows
    key_rows = jnp.arange(block_count, dtype=jnp.int32)[:, None, None] * band_rows - band_rows + key_idx[None]
    allowed = (distance >= 0)[None] & (distance <= band_rows)[None] & (key_rows >= 0)
    scores = jnp.where(allowed[:, None], scores, -jnp.inf)
    row_max = lax.optimization_barrier(jnp.max(scores, axis=-1, keepdims=True))
    numerators = jnp.exp(scores - row_max)
    row_sum = lax.optimization_barrier(jnp.sum(numerators, axis=-1, keepdims=True))
    rounded = lax.optimization_barrier(numerators.astype(jnp.bfloat16)).astype(jnp.float32)
    branch_out = jnp.einsum('nrqk,nkrd->nqrd', rounded, value_bands) / jnp.transpose(row_sum, (0, 2, 1, 3))
    log_total = jnp.transpose((row_max + jnp.log(row_sum))[..., 0], (0, 2, 1))
    return (branch_out.reshape(TOKENS, HEAD_DIM), log_total.reshape(TOKENS))

def one_head(operands):
    head_queries, head_keys, head_values = operands
    first_out, first_total = single_branch(head_queries, head_keys, head_values, W1, 1)
    second_output, second_branch_total = single_branch(head_queries, head_keys, head_values, WINDOW_TWO, DILATION_TWO)
    third_output, third_branch_total = single_branch(head_queries, head_keys, head_values, WINDOW_THREE, DILATION_THREE)
    weights = jax.nn.softmax(jnp.stack([first_total, second_branch_total, third_branch_total]), axis=0)
    stacked = jnp.stack([first_out, second_output, third_output])
    return lax.optimization_barrier(jnp.sum(weights[:, :, None] * stacked, axis=0))

def reference(queries, keys, values, w_out):
    per_head = lax.map(one_head, (jnp.transpose(queries, (1, 0, 2)), jnp.transpose(keys, (1, 0, 2)), jnp.transpose(values, (1, 0, 2))))
    attended = jnp.transpose(per_head, (1, 0, 2)).reshape(TOKENS, HEADS * HEAD_DIM).astype(jnp.bfloat16)
    return jnp.dot(attended, w_out, preferred_element_type=jnp.float32).astype(jnp.bfloat16)
```

```python
import functools
import math

import jax
import jax.numpy as jnp
from jax import lax
from jax.experimental import pallas as pl
from jax.experimental.pallas import tpu as pltpu
from jax.sharding import PartitionSpec as P

W1 = 128
WINDOW_TWO = 512
DILATION_TWO = 4
WINDOW_THREE = 2048
DILATION_THREE = 16
MESH = pl.DeviceIdType.MESH
RATIO = DILATION_THREE // DILATION_TWO
CHUNKS = DILATION_TWO
ROWS_ONE = 16
ROWS_TWO = WINDOW_TWO // DILATION_THREE


def attend(queries, keys, values, bias, scale):
    scores = lax.dot_general(
        queries, keys, (((1,), (1,)), ((), ())), preferred_element_type=jnp.float32
    )
    scores = scores * scale + bias
    top = jnp.max(scores, axis=-1, keepdims=True)
    numerators = jnp.exp2(scores - top)
    total = jnp.sum(numerators, axis=-1, keepdims=True)
    weighted = jnp.dot(numerators.astype(jnp.bfloat16), values, preferred_element_type=jnp.float32)
    return weighted, top, total


def bias_of(shape, place_q, place_k, first_own, window, has_prev):
    query_place, _ = place_q(lax.broadcasted_iota(jnp.int32, shape, 0))
    key_place, key_row = place_k(lax.broadcasted_iota(jnp.int32, shape, 1))
    distance = query_place - key_place
    allowed = (distance >= 0) & (distance <= window)
    general = jnp.where(allowed, 0.0, -jnp.inf).astype(jnp.float32)
    gate = jnp.where(has_prev, 0, first_own)
    first = jnp.where(allowed & (key_row >= gate), 0.0, -jnp.inf).astype(jnp.float32)
    return general, first


def kernel(
    group, q_ref, k_ref, v_ref, w_ref, o_ref,
    qb, kb, vb, acc, mx, sm, ob, ab, bias1, bias1f, bias2, bias2f, bias3,
    in_send, in_recv, z_send, z_recv, zl_send, zl_recv, o_send, o_recv, d_send, d_recv,
):
    res, dim = DILATION_THREE, q_ref.shape[-1]
    piece = q_ref.shape[2]
    rows = group * piece
    sp, tp = lax.axis_index("sp"), lax.axis_index("tp")
    n_sp, n_tp = lax.axis_size("sp"), lax.axis_size("tp")
    mine = lax.rem(sp, group)
    base = sp - mine
    has_prev = sp >= group
    has_next = sp + group < n_sp
    partner = n_tp - 1 - tp
    scale = math.log2(math.e) / math.sqrt(dim)

    barrier = pltpu.get_barrier_semaphore()
    for d in range(1, group):
        pl.semaphore_signal(
            barrier, inc=1, device_id={"sp": base + lax.rem(mine + d, group)}, device_id_type=MESH
        )
    pl.semaphore_signal(barrier, inc=1, device_id={"tp": partner}, device_id_type=MESH)

    @pl.when(has_prev)
    def _():
        pl.semaphore_signal(barrier, inc=1, device_id={"sp": sp - group}, device_id_type=MESH)

    @pl.when(has_next)
    def _():
        pl.semaphore_signal(barrier, inc=1, device_id={"sp": sp + group}, device_id_type=MESH)

    pl.semaphore_wait(barrier, group + jnp.where(has_prev, 1, 0) + jnp.where(has_next, 1, 0))

    def span(start):
        return pl.ds(pl.multiple_of(start, piece), piece)

    tensors = ((k_ref, kb, rows), (v_ref, vb, rows), (q_ref, qb, 0))

    def exchange(which, d):
        source, buffer, offset = tensors[which]
        other = lax.rem(mine + d, group)
        return pltpu.make_async_remote_copy(
            src_ref=source.at[other],
            dst_ref=buffer.at[:, span(offset + piece * mine), :],
            send_sem=in_send.at[which, d],
            recv_sem=in_recv.at[which, mine],
            device_id={"sp": base + other},
            device_id_type=MESH,
        )

    def arrival(which, origin):
        source, buffer, offset = tensors[which]
        return pltpu.make_async_remote_copy(
            src_ref=source.at[0],
            dst_ref=buffer.at[:, span(offset + piece * origin), :],
            send_sem=in_send.at[which, 0],
            recv_sem=in_recv.at[which, origin],
            device_id={"sp": sp},
            device_id_type=MESH,
        )

    def order(k):
        if k == 0:
            return mine
        high = group - k
        return jnp.where(high > mine, high, high - 1)

    def onward(which, k):
        source, buffer, _ = tensors[which]
        origin = order(k)
        src = source.at[mine] if k == 0 else buffer.at[:, span(rows + piece * origin), :]
        return pltpu.make_async_remote_copy(
            src_ref=src,
            dst_ref=buffer.at[:, span(piece * origin), :],
            send_sem=z_send.at[which, k],
            recv_sem=z_recv.at[which, k],
            device_id={"sp": sp + group},
            device_id_type=MESH,
        )

    def onward_last(which, s):
        _, buffer, _ = tensors[which]
        origin = order(group - 1)
        part = pl.ds(s * RATIO, RATIO)
        return pltpu.make_async_remote_copy(
            src_ref=buffer.at[part, span(rows + piece * origin), :],
            dst_ref=buffer.at[part, span(piece * origin), :],
            send_sem=zl_send.at[which, s],
            recv_sem=zl_recv.at[which, s],
            device_id={"sp": sp + group},
            device_id_type=MESH,
        )

    @pl.when(has_next)
    def _():
        for which in (0, 1):
            onward(which, 0).start()

    for which in (0, 1, 2):
        for d in range(1, group):
            exchange(which, d).start()

    for source, buffer, offset in tensors:
        buffer[:, span(offset + piece * mine), :] = source[mine]

    @pl.when(jnp.logical_not(has_prev))
    def _():
        kb[:, :rows, :] = jnp.zeros((res, rows, dim), kb.dtype)
        vb[:, :rows, :] = jnp.zeros((res, rows, dim), vb.dtype)

    def place_one(per):
        def place(i):
            store, row = i // per, i % per
            residue = (store % RATIO) * DILATION_TWO + store // RATIO
            return row * res + residue, row
        return place

    def place_two(per):
        def place(i):
            j, row = i // per, i % per
            return row * RATIO + j, row
        return place

    def shifted(place, by):
        def moved(i):
            at, row = place(i)
            return at + by, row
        return moved

    bias1[...], bias1f[...] = bias_of(
        bias1.shape, shifted(place_one(ROWS_ONE), ROWS_ONE * res), place_one(2 * ROWS_ONE), ROWS_ONE, W1, has_prev
    )
    bias2[...], bias2f[...] = bias_of(
        bias2.shape, shifted(place_two(ROWS_TWO), ROWS_TWO * RATIO), place_two(2 * ROWS_TWO), ROWS_TWO,
        WINDOW_TWO // DILATION_TWO, has_prev,
    )
    _, bias3[...] = bias_of(
        bias3.shape, lambda i: (i + rows, i), lambda i: (i, i), rows, WINDOW_THREE // DILATION_THREE, has_prev
    )

    for k in range(1, group):
        origin = order(k)
        for which in (0, 1):
            arrival(which, origin).wait_recv()

        @pl.when(has_next)
        def _():
            if k < group - 1:
                for which in (0, 1):
                    onward(which, k).start()
            else:
                for s in range(CHUNKS):
                    for which in (0, 1):
                        onward_last(which, s).start()

    for k in range(1, group):
        arrival(2, order(k)).wait_recv()

    def branch_one(b, bias):
        own = pl.ds(b * ROWS_ONE, ROWS_ONE)
        near = pl.ds(rows + (b - 1) * ROWS_ONE, 2 * ROWS_ONE)
        weighted, top, total = attend(
            qb[:, own, :].reshape(-1, dim), kb[:, near, :].reshape(-1, dim), vb[:, near, :].reshape(-1, dim),
            bias[...], scale,
        )
        acc[:, own, :] = weighted.reshape(res, ROWS_ONE, dim)
        mx[:, own, :] = top.reshape(res, ROWS_ONE, 1)
        sm[:, own, :] = total.reshape(res, ROWS_ONE, 1)

    def merge(at, weighted, top, total):
        old_top = mx[at].reshape(-1, 1)
        new_top = jnp.maximum(old_top, top)
        old_part, part = jnp.exp2(old_top - new_top), jnp.exp2(top - new_top)
        return (
            acc[at].reshape(-1, dim) * old_part + weighted * part,
            new_top,
            sm[at].reshape(-1, 1) * old_part + total * part,
        )

    def branch_two(s, b, bias):
        part = pl.ds(s * RATIO, RATIO)
        own = pl.ds(b * ROWS_TWO, ROWS_TWO)
        near = pl.ds(rows + (b - 1) * ROWS_TWO, 2 * ROWS_TWO)
        found = attend(
            qb[part, own, :].reshape(-1, dim), kb[part, near, :].reshape(-1, dim), vb[part, near, :].reshape(-1, dim),
            bias[...], scale,
        )
        at = (part, own, slice(None))
        weighted, top, total = merge(at, *found)
        acc[at] = weighted.reshape(RATIO, ROWS_TWO, dim)
        mx[at] = top.reshape(RATIO, ROWS_TWO, 1)
        sm[at] = total.reshape(RATIO, ROWS_TWO, 1)

    for b in range(1, rows // ROWS_ONE):
        branch_one(b, bias1)
    for s in range(CHUNKS):
        for b in range(1, rows // ROWS_TWO):
            branch_two(s, b, bias2)

    @pl.when(has_prev)
    def _():
        for k in range(group - 1):
            for which in (0, 1):
                onward(which, k).wait_recv()

    branch_one(0, bias1f)
    for s in range(CHUNKS):
        branch_two(s, 0, bias2f)

    head = tp * group + mine

    def lanes(index):
        return pl.ds(pl.multiple_of(index * dim, dim), dim)

    def give(s, d):
        part = pl.ds(s * RATIO, RATIO)
        other = lax.rem(mine + d, group)
        return pltpu.make_async_remote_copy(
            src_ref=ob.at[part, span(piece * other), :],
            dst_ref=ab.at[part, :, lanes(head)],
            send_sem=o_send.at[s, d],
            recv_sem=o_recv.at[s, mine],
            device_id={"sp": base + other},
            device_id_type=MESH,
        )

    def taken(s, origin):
        part = pl.ds(s * RATIO, RATIO)
        return pltpu.make_async_remote_copy(
            src_ref=ob.at[part, span(0), :],
            dst_ref=ab.at[part, :, lanes(tp * group + origin)],
            send_sem=o_send.at[s, 0],
            recv_sem=o_recv.at[s, origin],
            device_id={"sp": sp},
            device_id_type=MESH,
        )

    def swap(s, d):
        part = pl.ds(s * RATIO, RATIO)
        origin = lax.rem(mine + d, group)
        slot = ab.at[part, :, lanes(tp * group + origin)]
        return pltpu.make_async_remote_copy(
            src_ref=ob.at[part, span(piece * mine), :] if d == 0 else slot,
            dst_ref=slot,
            send_sem=d_send.at[s, d],
            recv_sem=d_recv.at[s, d],
            device_id={"tp": partner},
            device_id_type=MESH,
        )

    def swapped(s, d):
        part = pl.ds(s * RATIO, RATIO)
        origin = lax.rem(mine + d, group)
        return pltpu.make_async_remote_copy(
            src_ref=ob.at[part, span(0), :],
            dst_ref=ab.at[part, :, lanes(partner * group + origin)],
            send_sem=d_send.at[s, d],
            recv_sem=d_recv.at[s, d],
            device_id={"tp": partner},
            device_id_type=MESH,
        )

    for s in range(CHUNKS):
        part = pl.ds(s * RATIO, RATIO)

        @pl.when(has_prev)
        def _():
            for which in (0, 1):
                onward_last(which, s).wait_recv()

        for store in range(s * RATIO, (s + 1) * RATIO):
            found = attend(qb[store], kb[store], vb[store], bias3[...], scale)
            weighted, _, total = merge((store,), *found)
            ob[store] = (weighted / total).astype(ob.dtype)
        for d in range(1, group):
            give(s, d).start()
        swap(s, 0).start()
        ab[part, :, lanes(head)] = ob[part, span(piece * mine), :]

    for s in range(CHUNKS):
        part = pl.ds(s * RATIO, RATIO)
        for d in range(1, group):
            taken(s, lax.rem(mine + d, group)).wait_recv()
            swap(s, d).start()
    for s in range(CHUNKS):
        part = pl.ds(s * RATIO, RATIO)
        for d in range(group):
            swapped(s, d).wait_recv()
        attended = ab[part].reshape(RATIO * piece, -1)
        mixed = jnp.dot(attended, w_ref[...], preferred_element_type=jnp.float32)
        o_ref[part] = mixed.astype(o_ref.dtype).reshape(RATIO, piece, -1)

    for which in (0, 1, 2):
        for d in range(1, group):
            exchange(which, d).wait_send()

    @pl.when(has_next)
    def _():
        for which in (0, 1):
            for k in range(group - 1):
                onward(which, k).wait_send()
            for s in range(CHUNKS):
                onward_last(which, s).wait_send()

    for s in range(CHUNKS):
        for d in range(1, group):
            give(s, d).wait_send()
        for d in range(group):
            swap(s, d).wait_send()


def local(queries, keys, values, w_out):
    tokens, group, dim = queries.shape
    features, columns = w_out.shape
    res = DILATION_THREE
    piece = tokens // res
    rows = group * piece
    assert group * tokens == WINDOW_THREE and lax.axis_size("sp") % group == 0 and lax.axis_size("tp") == 2

    def by_residue(x):
        x = x.reshape(piece, RATIO, DILATION_TWO, group, dim)
        return jnp.transpose(x, (3, 2, 1, 0, 4)).reshape(group, res, piece, dim)

    low, full = jnp.bfloat16, jnp.float32
    dma = pltpu.SemaphoreType.DMA
    vmem = pl.BlockSpec(memory_space=pltpu.VMEM)
    mixed = pl.pallas_call(
        functools.partial(kernel, group),
        out_shape=jax.ShapeDtypeStruct((res, piece, columns), low),
        in_specs=[vmem] * 4,
        out_specs=vmem,
        scratch_shapes=[
            pltpu.VMEM((res, rows, dim), low),
            pltpu.VMEM((res, 2 * rows, dim), low),
            pltpu.VMEM((res, 2 * rows, dim), low),
            pltpu.VMEM((res, rows, dim), full),
            pltpu.VMEM((res, rows, 1), full),
            pltpu.VMEM((res, rows, 1), full),
            pltpu.VMEM((res, rows, dim), low),
            pltpu.VMEM((res, piece, features), low),
            pltpu.VMEM((res * ROWS_ONE, 2 * res * ROWS_ONE), full),
            pltpu.VMEM((res * ROWS_ONE, 2 * res * ROWS_ONE), full),
            pltpu.VMEM((RATIO * ROWS_TWO, 2 * RATIO * ROWS_TWO), full),
            pltpu.VMEM((RATIO * ROWS_TWO, 2 * RATIO * ROWS_TWO), full),
            pltpu.VMEM((rows, 2 * rows), full),
            dma((3, group)), dma((3, group)),
            dma((2, group)), dma((2, group)),
            dma((2, CHUNKS)), dma((2, CHUNKS)),
            dma((CHUNKS, group)), dma((CHUNKS, group)),
            dma((CHUNKS, group)), dma((CHUNKS, group)),
        ],
        compiler_params=pltpu.CompilerParams(
            collective_id=0, has_side_effects=True, vmem_limit_bytes=48 * 2**20
        ),
    )(by_residue(queries), by_residue(keys), by_residue(values), w_out)
    mixed = mixed.reshape(DILATION_TWO, RATIO, piece, columns)
    return jnp.transpose(mixed, (2, 1, 0, 3)).reshape(tokens, columns)


def solution(mesh):
    in_specs = (P("sp", "tp", None), P("sp", "tp", None), P("sp", "tp", None), P(None, "tp"))
    out_specs = P("sp", "tp")
    return jax.shard_map(local, mesh=mesh, in_specs=in_specs, out_specs=out_specs, check_vma=False)
```

```python
import functools
import math

import jax
import jax.numpy as jnp
from jax import lax
from jax.experimental import pallas as pl
from jax.experimental.pallas import tpu as pltpu
from jax.sharding import PartitionSpec as P

W1 = 128
WINDOW_TWO = 512
DILATION_TWO = 4
WINDOW_THREE = 2048
DILATION_THREE = 16
MESH = pl.DeviceIdType.MESH
RATIO = DILATION_THREE // DILATION_TWO
CHUNKS = DILATION_TWO
ROWS_ONE = 16
ROWS_TWO = WINDOW_TWO // DILATION_THREE


def attend(blocks, scale):
    scores = [
        lax.dot_general(q, k, (((1,), (1,)), ((), ())), preferred_element_type=jnp.float32)
        for q, k, _, _ in blocks
    ]
    scores = [x * scale + bias for x, (_, _, _, bias) in zip(scores, blocks)]
    tops = [jnp.max(x, axis=-1, keepdims=True) for x in scores]
    numerators = [jnp.exp2(x - top) for x, top in zip(scores, tops)]
    totals = [jnp.sum(x, axis=-1, keepdims=True) for x in numerators]
    weighted = [
        jnp.dot(x.astype(jnp.bfloat16), v, preferred_element_type=jnp.float32)
        for x, (_, _, v, _) in zip(numerators, blocks)
    ]
    return list(zip(weighted, tops, totals))


def bias_of(shape, place_q, place_k, first_own, window, has_prev):
    query_place, _ = place_q(lax.broadcasted_iota(jnp.int32, shape, 0))
    key_place, key_row = place_k(lax.broadcasted_iota(jnp.int32, shape, 1))
    distance = query_place - key_place
    allowed = (distance >= 0) & (distance <= window)
    general = jnp.where(allowed, 0.0, -jnp.inf).astype(jnp.float32)
    gate = jnp.where(has_prev, 0, first_own)
    first = jnp.where(allowed & (key_row >= gate), 0.0, -jnp.inf).astype(jnp.float32)
    return general, first


def kernel(
    group, q_ref, k_ref, v_ref, w_ref, o_ref,
    qb, kb, vb, acc, mx, sm, ob, ab, bias1, bias1f, bias2, bias2f, bias3,
    in_send, in_recv, z_send, z_recv, zl_send, zl_recv, o_send, o_recv, d_send, d_recv,
):
    res, dim = DILATION_THREE, q_ref.shape[-1]
    piece = q_ref.shape[2]
    rows = group * piece
    sp, tp = lax.axis_index("sp"), lax.axis_index("tp")
    n_sp, n_tp = lax.axis_size("sp"), lax.axis_size("tp")
    mine = lax.rem(sp, group)
    base = sp - mine
    has_prev = sp >= group
    has_next = sp + group < n_sp
    partner = n_tp - 1 - tp
    scale = math.log2(math.e) / math.sqrt(dim)

    barrier = pltpu.get_barrier_semaphore()
    for d in range(1, group):
        pl.semaphore_signal(
            barrier, inc=1, device_id={"sp": base + lax.rem(mine + d, group)}, device_id_type=MESH
        )
    pl.semaphore_signal(barrier, inc=1, device_id={"tp": partner}, device_id_type=MESH)

    @pl.when(has_prev)
    def _():
        pl.semaphore_signal(barrier, inc=1, device_id={"sp": sp - group}, device_id_type=MESH)

    @pl.when(has_next)
    def _():
        pl.semaphore_signal(barrier, inc=1, device_id={"sp": sp + group}, device_id_type=MESH)

    pl.semaphore_wait(barrier, group + jnp.where(has_prev, 1, 0) + jnp.where(has_next, 1, 0))

    def span(start):
        return pl.ds(pl.multiple_of(start, piece), piece)

    tensors = ((k_ref, kb, rows), (v_ref, vb, rows), (q_ref, qb, 0))

    def member(d):
        other, bit = mine, 1
        while bit <= d:
            if d & bit:
                other = other + bit * (1 - 2 * lax.rem(mine // bit, 2))
            bit *= 2
        return other

    def exchange(which, d):
        source, buffer, offset = tensors[which]
        other = member(d)
        return pltpu.make_async_remote_copy(
            src_ref=source.at[other],
            dst_ref=buffer.at[:, span(offset + piece * mine), :],
            send_sem=in_send.at[which, d],
            recv_sem=in_recv.at[which, d],
            device_id={"sp": base + other},
            device_id_type=MESH,
        )

    def arrival(which, d):
        source, buffer, offset = tensors[which]
        return pltpu.make_async_remote_copy(
            src_ref=source.at[0],
            dst_ref=buffer.at[:, span(offset + piece * member(d)), :],
            send_sem=in_send.at[which, d],
            recv_sem=in_recv.at[which, d],
            device_id={"sp": sp},
            device_id_type=MESH,
        )

    low = piece - ROWS_ONE

    def onward_rows(which, k):
        source, buffer, _ = tensors[which]
        start = piece * member(k)
        if k == 0:
            src, dst = source.at[mine], buffer.at[:, span(start), :]
        elif k in whole:
            src, dst = buffer.at[:, span(rows + start), :], buffer.at[:, span(start), :]
        else:
            ends = [pl.ds(pl.multiple_of(x + start + low, ROWS_ONE), ROWS_ONE) for x in (rows, 0)]
            src, dst = (buffer.at[:, x, :] for x in ends)
        return pltpu.make_async_remote_copy(
            src_ref=src,
            dst_ref=dst,
            send_sem=z_send.at[which, k],
            recv_sem=z_recv.at[which, k],
            device_id={"sp": sp + group},
            device_id_type=MESH,
        )

    def onward_chunk(which, k, s):
        _, buffer, _ = tensors[which]
        start = piece * member(k)
        part = pl.ds(s * RATIO, RATIO)
        return pltpu.make_async_remote_copy(
            src_ref=buffer.at[part, pl.ds(pl.multiple_of(rows + start, ROWS_ONE), low), :],
            dst_ref=buffer.at[part, pl.ds(pl.multiple_of(start, ROWS_ONE), low), :],
            send_sem=zl_send.at[which, k, s],
            recv_sem=zl_recv.at[which, k, s],
            device_id={"sp": sp + group},
            device_id_type=MESH,
        )

    whole = range(group // 2)
    split = range(group // 2, group)

    @pl.when(has_next)
    def _():
        for which in (0, 1):
            onward_rows(which, 0).start()

    near = [d for d in range(1, group) if d & (d - 1) == 0]
    far = [d for d in range(1, group) if d & (d - 1)]
    for tensors_now in ((0, 1), (2,)):
        for members in (near, far):
            for which in tensors_now:
                for d in members:
                    exchange(which, d).start()

    for source, buffer, offset in tensors:
        buffer[:, span(offset + piece * mine), :] = source[mine]

    @pl.when(jnp.logical_not(has_prev))
    def _():
        kb[:, :rows, :] = jnp.zeros((res, rows, dim), kb.dtype)
        vb[:, :rows, :] = jnp.zeros((res, rows, dim), vb.dtype)

    def place_one(per):
        def place(i):
            store, row = i // per, i % per
            residue = (store % RATIO) * DILATION_TWO + store // RATIO
            return row * res + residue, row
        return place

    def place_two(per):
        def place(i):
            j, row = i // per, i % per
            return row * RATIO + j, row
        return place

    def shifted(place, by):
        def moved(i):
            at, row = place(i)
            return at + by, row
        return moved

    bias1[...], bias1f[...] = bias_of(
        bias1.shape, shifted(place_one(ROWS_ONE), ROWS_ONE * res), place_one(2 * ROWS_ONE), ROWS_ONE, W1, has_prev
    )
    bias2[...], bias2f[...] = bias_of(
        bias2.shape, shifted(place_two(ROWS_TWO), ROWS_TWO * RATIO), place_two(2 * ROWS_TWO), ROWS_TWO,
        WINDOW_TWO // DILATION_TWO, has_prev,
    )
    _, bias3[...] = bias_of(
        bias3.shape, lambda i: (i + rows, i), lambda i: (i, i), rows, WINDOW_THREE // DILATION_THREE, has_prev
    )

    for k in range(1, group):
        for which in (0, 1):
            arrival(which, k).wait_recv()

        @pl.when(has_next)
        def _():
            for which in (0, 1):
                onward_rows(which, k).start()

    @pl.when(has_next)
    def _():
        for s in range(CHUNKS):
            for k in split:
                for which in (0, 1):
                    onward_chunk(which, k, s).start()

    for k in range(1, group):
        arrival(2, k).wait_recv()

    def branch_one(blocks, bias):
        spans = [
            (pl.ds(b * ROWS_ONE, ROWS_ONE), pl.ds(rows + (b - 1) * ROWS_ONE, 2 * ROWS_ONE)) for b in blocks
        ]
        found = attend(
            [
                tuple(x[:, at, :].reshape(-1, dim) for x, at in ((qb, own), (kb, near), (vb, near))) + (bias[...],)
                for own, near in spans
            ],
            scale,
        )
        for (own, _), (weighted, top, total) in zip(spans, found):
            acc[:, own, :] = weighted.reshape(res, ROWS_ONE, dim)
            mx[:, own, :] = top.reshape(res, ROWS_ONE, 1)
            sm[:, own, :] = total.reshape(res, ROWS_ONE, 1)

    def merge(at, weighted, top, total):
        old_top = mx[at].reshape(-1, 1)
        new_top = jnp.maximum(old_top, top)
        old_part, part = jnp.exp2(old_top - new_top), jnp.exp2(top - new_top)
        return (
            acc[at].reshape(-1, dim) * old_part + weighted * part,
            new_top,
            sm[at].reshape(-1, 1) * old_part + total * part,
        )

    def branch_two(blocks, bias):
        spans = [
            (
                pl.ds(s * RATIO, RATIO),
                pl.ds(b * ROWS_TWO, ROWS_TWO),
                pl.ds(rows + (b - 1) * ROWS_TWO, 2 * ROWS_TWO),
            )
            for s, b in blocks
        ]
        found = attend(
            [
                tuple(x[part, at, :].reshape(-1, dim) for x, at in ((qb, own), (kb, near), (vb, near))) + (bias[...],)
                for part, own, near in spans
            ],
            scale,
        )
        merged = [merge((part, own, slice(None)), *one) for (part, own, _), one in zip(spans, found)]
        for (part, own, _), (weighted, top, total) in zip(spans, merged):
            acc[part, own, :] = weighted.reshape(RATIO, ROWS_TWO, dim)
            mx[part, own, :] = top.reshape(RATIO, ROWS_TWO, 1)
            sm[part, own, :] = total.reshape(RATIO, ROWS_TWO, 1)

    def some(items, count):
        return [items[i : i + count] for i in range(0, len(items), count)]

    for blocks in some(list(range(1, rows // ROWS_ONE)), 2):
        branch_one(blocks, bias1)
    for blocks in some([(s, b) for s in range(CHUNKS) for b in range(1, rows // ROWS_TWO)], 4):
        branch_two(blocks, bias2)

    @pl.when(has_prev)
    def _():
        for k in range(group):
            for which in (0, 1):
                onward_rows(which, k).wait_recv()

    branch_one([0], bias1f)

    head = tp * group + mine

    def lanes(index):
        return pl.ds(pl.multiple_of(index * dim, dim), dim)

    def give(s, d):
        part = pl.ds(s * RATIO, RATIO)
        other = member(d)
        return pltpu.make_async_remote_copy(
            src_ref=ob.at[part, span(piece * other), :],
            dst_ref=ab.at[part, :, lanes(head)],
            send_sem=o_send.at[s, d],
            recv_sem=o_recv.at[s, d],
            device_id={"sp": base + other},
            device_id_type=MESH,
        )

    def taken(s, d):
        part = pl.ds(s * RATIO, RATIO)
        return pltpu.make_async_remote_copy(
            src_ref=ob.at[part, span(0), :],
            dst_ref=ab.at[part, :, lanes(tp * group + member(d))],
            send_sem=o_send.at[s, d],
            recv_sem=o_recv.at[s, d],
            device_id={"sp": sp},
            device_id_type=MESH,
        )

    def swap(s, d):
        part = pl.ds(s * RATIO, RATIO)
        slot = ab.at[part, :, lanes(tp * group + member(d))]
        return pltpu.make_async_remote_copy(
            src_ref=ob.at[part, span(piece * mine), :] if d == 0 else slot,
            dst_ref=slot,
            send_sem=d_send.at[s, d],
            recv_sem=d_recv.at[s, d],
            device_id={"tp": partner},
            device_id_type=MESH,
        )

    def swapped(s, d):
        part = pl.ds(s * RATIO, RATIO)
        return pltpu.make_async_remote_copy(
            src_ref=ob.at[part, span(0), :],
            dst_ref=ab.at[part, :, lanes(partner * group + member(d))],
            send_sem=d_send.at[s, d],
            recv_sem=d_recv.at[s, d],
            device_id={"tp": partner},
            device_id_type=MESH,
        )

    def hand_over(s):
        for d in range(1, group):
            taken(s, d).wait_recv()
            swap(s, d).start()

    def project(s):
        part = pl.ds(s * RATIO, RATIO)
        for d in range(group):
            swapped(s, d).wait_recv()
        attended = ab[part].reshape(RATIO * piece, -1)
        mixed = jnp.dot(attended, w_ref[...], preferred_element_type=jnp.float32)
        o_ref[part] = mixed.astype(o_ref.dtype).reshape(RATIO, piece, -1)

    for s in range(CHUNKS):
        part = pl.ds(s * RATIO, RATIO)

        @pl.when(has_prev)
        def _():
            for k in split:
                for which in (0, 1):
                    onward_chunk(which, k, s).wait_recv()

        branch_two([(s, 0)], bias2f)
        stores = range(s * RATIO, (s + 1) * RATIO)
        found = attend([(qb[x], kb[x], vb[x], bias3[...]) for x in stores], scale)
        for x, one in zip(stores, found):
            weighted, _, total = merge((x,), *one)
            ob[x] = (weighted / total).astype(ob.dtype)
        for d in far + near:
            give(s, d).start()
        swap(s, 0).start()
        ab[part, :, lanes(head)] = ob[part, span(piece * mine), :]
        if s >= 2:
            hand_over(s - 2)
    for s in range(CHUNKS - 2, CHUNKS):
        hand_over(s)
        project(s - 2)
    for s in range(CHUNKS - 2, CHUNKS):
        project(s)

    for which in (0, 1, 2):
        for d in range(1, group):
            exchange(which, d).wait_send()

    @pl.when(has_next)
    def _():
        for which in (0, 1):
            for k in range(group):
                onward_rows(which, k).wait_send()
            for k in split:
                for s in range(CHUNKS):
                    onward_chunk(which, k, s).wait_send()

    for s in range(CHUNKS):
        for d in range(1, group):
            give(s, d).wait_send()
        for d in range(group):
            swap(s, d).wait_send()


def local(queries, keys, values, w_out):
    tokens, group, dim = queries.shape
    features, columns = w_out.shape
    res = DILATION_THREE
    piece = tokens // res
    rows = group * piece
    assert group & (group - 1) == 0 and piece > ROWS_ONE
    assert group * tokens == WINDOW_THREE and lax.axis_size("sp") % group == 0 and lax.axis_size("tp") == 2

    def by_residue(x):
        x = x.reshape(piece, RATIO, DILATION_TWO, group, dim)
        return jnp.transpose(x, (3, 2, 1, 0, 4)).reshape(group, res, piece, dim)

    low, full = jnp.bfloat16, jnp.float32
    dma = pltpu.SemaphoreType.DMA
    vmem = pl.BlockSpec(memory_space=pltpu.VMEM)
    mixed = pl.pallas_call(
        functools.partial(kernel, group),
        out_shape=jax.ShapeDtypeStruct((res, piece, columns), low),
        in_specs=[vmem] * 4,
        out_specs=vmem,
        scratch_shapes=[
            pltpu.VMEM((res, rows, dim), low),
            pltpu.VMEM((res, 2 * rows, dim), low),
            pltpu.VMEM((res, 2 * rows, dim), low),
            pltpu.VMEM((res, rows, dim), full),
            pltpu.VMEM((res, rows, 1), full),
            pltpu.VMEM((res, rows, 1), full),
            pltpu.VMEM((res, rows, dim), low),
            pltpu.VMEM((res, piece, features), low),
            pltpu.VMEM((res * ROWS_ONE, 2 * res * ROWS_ONE), full),
            pltpu.VMEM((res * ROWS_ONE, 2 * res * ROWS_ONE), full),
            pltpu.VMEM((RATIO * ROWS_TWO, 2 * RATIO * ROWS_TWO), full),
            pltpu.VMEM((RATIO * ROWS_TWO, 2 * RATIO * ROWS_TWO), full),
            pltpu.VMEM((rows, 2 * rows), full),
            dma((3, group)), dma((3, group)),
            dma((2, group)), dma((2, group)),
            dma((2, group, CHUNKS)), dma((2, group, CHUNKS)),
            dma((CHUNKS, group)), dma((CHUNKS, group)),
            dma((CHUNKS, group)), dma((CHUNKS, group)),
        ],
        compiler_params=pltpu.CompilerParams(
            collective_id=0, has_side_effects=True, vmem_limit_bytes=48 * 2**20
        ),
    )(by_residue(queries), by_residue(keys), by_residue(values), w_out)
    mixed = mixed.reshape(DILATION_TWO, RATIO, piece, columns)
    return jnp.transpose(mixed, (2, 1, 0, 3)).reshape(tokens, columns)


def solution(mesh):
    in_specs = (P("sp", "tp", None), P("sp", "tp", None), P("sp", "tp", None), P(None, "tp"))
    out_specs = P("sp", "tp")
    return jax.shard_map(local, mesh=mesh, in_specs=in_specs, out_specs=out_specs, check_vma=False)
```

```python
import functools
import math

import jax
import jax.numpy as jnp
from jax import lax
from jax.experimental import pallas as pl
from jax.experimental.pallas import tpu as pltpu
from jax.sharding import PartitionSpec as P

W1 = 128
WINDOW_TWO = 512
DILATION_TWO = 4
WINDOW_THREE = 2048
DILATION_THREE = 16
MESH = pl.DeviceIdType.MESH
RATIO = DILATION_THREE // DILATION_TWO
CHUNKS = DILATION_TWO
ROWS_ONE = 16
ROWS_TWO = WINDOW_TWO // DILATION_THREE


def attend(blocks, scale):
    scores = [
        lax.dot_general(q, k, (((1,), (1,)), ((), ())), preferred_element_type=jnp.float32)
        for q, k, _, _ in blocks
    ]
    scores = [x * scale + bias for x, (_, _, _, bias) in zip(scores, blocks)]
    tops = [jnp.max(x, axis=-1, keepdims=True) for x in scores]
    numerators = [jnp.exp2(x - top) for x, top in zip(scores, tops)]
    sums = [
        jnp.dot(
            x.astype(v.dtype), jnp.concatenate([v, jnp.ones_like(v)], axis=1), preferred_element_type=jnp.float32
        )
        for x, (_, _, v, _) in zip(numerators, blocks)
    ]
    dim = blocks[0][2].shape[-1]
    return [(x[:, :dim], jnp.broadcast_to(top, x[:, :dim].shape), x[:, dim:]) for x, top in zip(sums, tops)]


def bias_of(shape, place_q, place_k, first_own, window, has_prev):
    query_place, _ = place_q(lax.broadcasted_iota(jnp.int32, shape, 0))
    key_place, key_row = place_k(lax.broadcasted_iota(jnp.int32, shape, 1))
    distance = query_place - key_place
    allowed = (distance >= 0) & (distance <= window)
    general = jnp.where(allowed, 0.0, -jnp.inf).astype(jnp.float32)
    gate = jnp.where(has_prev, 0, first_own)
    first = jnp.where(allowed & (key_row >= gate), 0.0, -jnp.inf).astype(jnp.float32)
    return general, first


def kernel(
    group, q_ref, k_ref, v_ref, w_ref, o_ref,
    qb, kb, vb, acc, mx, sm, ob, ab, bias1, bias1f, bias2, bias2f, bias3,
    in_send, in_recv, z_send, z_recv, zl_send, zl_recv, o_send, o_recv, d_send, d_recv,
):
    res, dim = DILATION_THREE, q_ref.shape[-1]
    piece = q_ref.shape[2]
    rows = group * piece
    sp, tp = lax.axis_index("sp"), lax.axis_index("tp")
    n_sp, n_tp = lax.axis_size("sp"), lax.axis_size("tp")
    mine = lax.rem(sp, group)
    base = sp - mine
    has_prev = sp >= group
    has_next = sp + group < n_sp
    partner = n_tp - 1 - tp
    scale = math.log2(math.e) / math.sqrt(dim)

    barrier = pltpu.get_barrier_semaphore()
    for d in range(1, group):
        pl.semaphore_signal(
            barrier, inc=1, device_id={"sp": base + lax.rem(mine + d, group)}, device_id_type=MESH
        )
    pl.semaphore_signal(barrier, inc=1, device_id={"tp": partner}, device_id_type=MESH)

    @pl.when(has_prev)
    def _():
        pl.semaphore_signal(barrier, inc=1, device_id={"sp": sp - group}, device_id_type=MESH)

    @pl.when(has_next)
    def _():
        pl.semaphore_signal(barrier, inc=1, device_id={"sp": sp + group}, device_id_type=MESH)

    pl.semaphore_wait(barrier, group + jnp.where(has_prev, 1, 0) + jnp.where(has_next, 1, 0))

    def span(start):
        return pl.ds(pl.multiple_of(start, piece), piece)

    tensors = ((k_ref, kb, rows), (v_ref, vb, rows), (q_ref, qb, 0))

    def member(d):
        other, bit = mine, 1
        while bit <= d:
            if d & bit:
                other = other + bit * (1 - 2 * lax.rem(mine // bit, 2))
            bit *= 2
        return other

    def exchange(which, d):
        source, buffer, offset = tensors[which]
        other = member(d)
        return pltpu.make_async_remote_copy(
            src_ref=source.at[other],
            dst_ref=buffer.at[:, span(offset + piece * mine), :],
            send_sem=in_send.at[which, d],
            recv_sem=in_recv.at[which, d],
            device_id={"sp": base + other},
            device_id_type=MESH,
        )

    def arrival(which, d):
        source, buffer, offset = tensors[which]
        return pltpu.make_async_remote_copy(
            src_ref=source.at[0],
            dst_ref=buffer.at[:, span(offset + piece * member(d)), :],
            send_sem=in_send.at[which, d],
            recv_sem=in_recv.at[which, d],
            device_id={"sp": sp},
            device_id_type=MESH,
        )

    low = piece - ROWS_ONE

    def onward_rows(which, k):
        source, buffer, _ = tensors[which]
        start = piece * member(k)
        if k == 0:
            src, dst = source.at[mine], buffer.at[:, span(start), :]
        elif k in whole:
            src, dst = buffer.at[:, span(rows + start), :], buffer.at[:, span(start), :]
        else:
            ends = [pl.ds(pl.multiple_of(x + start + low, ROWS_ONE), ROWS_ONE) for x in (rows, 0)]
            src, dst = (buffer.at[:, x, :] for x in ends)
        return pltpu.make_async_remote_copy(
            src_ref=src,
            dst_ref=dst,
            send_sem=z_send.at[which, k],
            recv_sem=z_recv.at[which, k],
            device_id={"sp": sp + group},
            device_id_type=MESH,
        )

    def onward_chunk(which, k, s):
        _, buffer, _ = tensors[which]
        start = piece * member(k)
        part = pl.ds(s * RATIO, RATIO)
        return pltpu.make_async_remote_copy(
            src_ref=buffer.at[part, pl.ds(pl.multiple_of(rows + start, ROWS_ONE), low), :],
            dst_ref=buffer.at[part, pl.ds(pl.multiple_of(start, ROWS_ONE), low), :],
            send_sem=zl_send.at[which, k, s],
            recv_sem=zl_recv.at[which, k, s],
            device_id={"sp": sp + group},
            device_id_type=MESH,
        )

    whole = range(group // 2)
    split = range(group // 2, group)

    @pl.when(has_next)
    def _():
        for which in (0, 1):
            onward_rows(which, 0).start()

    near = [d for d in range(1, group) if d & (d - 1) == 0]
    far = [d for d in range(1, group) if d & (d - 1)]
    for tensors_now in ((0, 1), (2,)):
        for members in (near, far):
            for which in tensors_now:
                for d in members:
                    exchange(which, d).start()

    for source, buffer, offset in tensors:
        buffer[:, span(offset + piece * mine), :] = source[mine]

    @pl.when(jnp.logical_not(has_prev))
    def _():
        kb[:, :rows, :] = jnp.zeros((res, rows, dim), kb.dtype)
        vb[:, :rows, :] = jnp.zeros((res, rows, dim), vb.dtype)

    def place_one(per):
        def place(i):
            store, row = i // per, i % per
            residue = (store % RATIO) * DILATION_TWO + store // RATIO
            return row * res + residue, row
        return place

    def place_two(per):
        def place(i):
            j, row = i // per, i % per
            return row * RATIO + j, row
        return place

    def shifted(place, by):
        def moved(i):
            at, row = place(i)
            return at + by, row
        return moved

    bias1[...], bias1f[...] = bias_of(
        bias1.shape, shifted(place_one(ROWS_ONE), ROWS_ONE * res), place_one(2 * ROWS_ONE), ROWS_ONE, W1, has_prev
    )
    bias2[...], bias2f[...] = bias_of(
        bias2.shape, shifted(place_two(ROWS_TWO), ROWS_TWO * RATIO), place_two(2 * ROWS_TWO), ROWS_TWO,
        WINDOW_TWO // DILATION_TWO, has_prev,
    )
    _, bias3[...] = bias_of(
        bias3.shape, lambda i: (i + rows, i), lambda i: (i, i), rows, WINDOW_THREE // DILATION_THREE, has_prev
    )

    for k in range(1, group):
        for which in (0, 1):
            arrival(which, k).wait_recv()

        @pl.when(has_next)
        def _():
            for which in (0, 1):
                onward_rows(which, k).start()

    @pl.when(has_next)
    def _():
        for s in range(CHUNKS):
            for k in split:
                for which in (0, 1):
                    onward_chunk(which, k, s).start()

    for k in range(1, group):
        arrival(2, k).wait_recv()

    def branch_one(blocks, bias):
        spans = [
            (pl.ds(b * ROWS_ONE, ROWS_ONE), pl.ds(rows + (b - 1) * ROWS_ONE, 2 * ROWS_ONE)) for b in blocks
        ]
        found = attend(
            [
                tuple(x[:, at, :].reshape(-1, dim) for x, at in ((qb, own), (kb, near), (vb, near))) + (bias[...],)
                for own, near in spans
            ],
            scale,
        )
        for (own, _), (weighted, top, total) in zip(spans, found):
            acc[:, own, :] = weighted.reshape(res, ROWS_ONE, dim)
            mx[:, own, :] = top.reshape(res, ROWS_ONE, dim)
            sm[:, own, :] = total.reshape(res, ROWS_ONE, dim)

    def merge(at, weighted, top, total):
        old_top = mx[at].reshape(-1, dim)
        new_top = jnp.maximum(old_top, top)
        old_part, part = jnp.exp2(old_top - new_top), jnp.exp2(top - new_top)
        return (
            acc[at].reshape(-1, dim) * old_part + weighted * part,
            new_top,
            sm[at].reshape(-1, dim) * old_part + total * part,
        )

    def branch_two(blocks, bias):
        spans = [
            (
                pl.ds(s * RATIO, RATIO),
                pl.ds(b * ROWS_TWO, ROWS_TWO),
                pl.ds(rows + (b - 1) * ROWS_TWO, 2 * ROWS_TWO),
            )
            for s, b in blocks
        ]
        found = attend(
            [
                tuple(x[part, at, :].reshape(-1, dim) for x, at in ((qb, own), (kb, near), (vb, near))) + (bias[...],)
                for part, own, near in spans
            ],
            scale,
        )
        merged = [merge((part, own, slice(None)), *one) for (part, own, _), one in zip(spans, found)]
        for (part, own, _), (weighted, top, total) in zip(spans, merged):
            acc[part, own, :] = weighted.reshape(RATIO, ROWS_TWO, dim)
            mx[part, own, :] = top.reshape(RATIO, ROWS_TWO, dim)
            sm[part, own, :] = total.reshape(RATIO, ROWS_TWO, dim)

    def some(items, count):
        return [items[i : i + count] for i in range(0, len(items), count)]

    for blocks in some(list(range(1, rows // ROWS_ONE)), 1):
        branch_one(blocks, bias1)
    for blocks in some([(s, b) for s in range(CHUNKS) for b in range(1, rows // ROWS_TWO)], 2):
        branch_two(blocks, bias2)

    @pl.when(has_prev)
    def _():
        for k in range(group):
            for which in (0, 1):
                onward_rows(which, k).wait_recv()

    branch_one([0], bias1f)

    head = tp * group + mine

    def lanes(index):
        return pl.ds(pl.multiple_of(index * dim, dim), dim)

    def give(s, d):
        part = pl.ds(s * RATIO, RATIO)
        other = member(d)
        return pltpu.make_async_remote_copy(
            src_ref=ob.at[part, span(piece * other), :],
            dst_ref=ab.at[part, :, lanes(head)],
            send_sem=o_send.at[s, d],
            recv_sem=o_recv.at[s, d],
            device_id={"sp": base + other},
            device_id_type=MESH,
        )

    def taken(s, d):
        part = pl.ds(s * RATIO, RATIO)
        return pltpu.make_async_remote_copy(
            src_ref=ob.at[part, span(0), :],
            dst_ref=ab.at[part, :, lanes(tp * group + member(d))],
            send_sem=o_send.at[s, d],
            recv_sem=o_recv.at[s, d],
            device_id={"sp": sp},
            device_id_type=MESH,
        )

    def swap(s, d):
        part = pl.ds(s * RATIO, RATIO)
        slot = ab.at[part, :, lanes(tp * group + member(d))]
        return pltpu.make_async_remote_copy(
            src_ref=ob.at[part, span(piece * mine), :] if d == 0 else slot,
            dst_ref=slot,
            send_sem=d_send.at[s, d],
            recv_sem=d_recv.at[s, d],
            device_id={"tp": partner},
            device_id_type=MESH,
        )

    def swapped(s, d):
        part = pl.ds(s * RATIO, RATIO)
        return pltpu.make_async_remote_copy(
            src_ref=ob.at[part, span(0), :],
            dst_ref=ab.at[part, :, lanes(partner * group + member(d))],
            send_sem=d_send.at[s, d],
            recv_sem=d_recv.at[s, d],
            device_id={"tp": partner},
            device_id_type=MESH,
        )

    def hand_over(s):
        for d in range(1, group):
            taken(s, d).wait_recv()
            swap(s, d).start()

    def project(s):
        part = pl.ds(s * RATIO, RATIO)
        for d in range(group):
            swapped(s, d).wait_recv()
        attended = ab[part].reshape(RATIO * piece, -1)
        mixed = jnp.dot(attended, w_ref[...], preferred_element_type=jnp.float32)
        o_ref[part] = mixed.astype(o_ref.dtype).reshape(RATIO, piece, -1)

    for s in range(CHUNKS):
        part = pl.ds(s * RATIO, RATIO)

        @pl.when(has_prev)
        def _():
            for k in split:
                for which in (0, 1):
                    onward_chunk(which, k, s).wait_recv()

        branch_two([(s, 0)], bias2f)
        for stores in some(list(range(s * RATIO, (s + 1) * RATIO)), 2):
            found = attend([(qb[x], kb[x], vb[x], bias3[...]) for x in stores], scale)
            for x, one in zip(stores, found):
                weighted, _, total = merge((x,), *one)
                ob[x] = (weighted / total).astype(ob.dtype)
        for d in far + near:
            give(s, d).start()
        swap(s, 0).start()
        ab[part, :, lanes(head)] = ob[part, span(piece * mine), :]
        if s >= 2:
            hand_over(s - 2)
    for s in range(CHUNKS - 2, CHUNKS):
        hand_over(s)
        project(s - 2)
    for s in range(CHUNKS - 2, CHUNKS):
        project(s)

    for which in (0, 1, 2):
        for d in range(1, group):
            exchange(which, d).wait_send()

    @pl.when(has_next)
    def _():
        for which in (0, 1):
            for k in range(group):
                onward_rows(which, k).wait_send()
            for k in split:
                for s in range(CHUNKS):
                    onward_chunk(which, k, s).wait_send()

    for s in range(CHUNKS):
        for d in range(1, group):
            give(s, d).wait_send()
        for d in range(group):
            swap(s, d).wait_send()


def local(queries, keys, values, w_out):
    tokens, group, dim = queries.shape
    features, columns = w_out.shape
    res = DILATION_THREE
    piece = tokens // res
    rows = group * piece
    assert group & (group - 1) == 0 and piece > ROWS_ONE
    assert group * tokens == WINDOW_THREE and lax.axis_size("sp") % group == 0 and lax.axis_size("tp") == 2

    def by_residue(x):
        x = x.reshape(piece, RATIO, DILATION_TWO, group, dim)
        return jnp.transpose(x, (3, 2, 1, 0, 4)).reshape(group, res, piece, dim)

    low, full = jnp.bfloat16, jnp.float32
    dma = pltpu.SemaphoreType.DMA
    vmem = pl.BlockSpec(memory_space=pltpu.VMEM)
    mixed = pl.pallas_call(
        functools.partial(kernel, group),
        out_shape=jax.ShapeDtypeStruct((res, piece, columns), low),
        in_specs=[vmem] * 4,
        out_specs=vmem,
        scratch_shapes=[
            pltpu.VMEM((res, rows, dim), low),
            pltpu.VMEM((res, 2 * rows, dim), low),
            pltpu.VMEM((res, 2 * rows, dim), low),
            pltpu.VMEM((res, rows, dim), full),
            pltpu.VMEM((res, rows, dim), full),
            pltpu.VMEM((res, rows, dim), full),
            pltpu.VMEM((res, rows, dim), low),
            pltpu.VMEM((res, piece, features), low),
            pltpu.VMEM((res * ROWS_ONE, 2 * res * ROWS_ONE), full),
            pltpu.VMEM((res * ROWS_ONE, 2 * res * ROWS_ONE), full),
            pltpu.VMEM((RATIO * ROWS_TWO, 2 * RATIO * ROWS_TWO), full),
            pltpu.VMEM((RATIO * ROWS_TWO, 2 * RATIO * ROWS_TWO), full),
            pltpu.VMEM((rows, 2 * rows), full),
            dma((3, group)), dma((3, group)),
            dma((2, group)), dma((2, group)),
            dma((2, group, CHUNKS)), dma((2, group, CHUNKS)),
            dma((CHUNKS, group)), dma((CHUNKS, group)),
            dma((CHUNKS, group)), dma((CHUNKS, group)),
        ],
        compiler_params=pltpu.CompilerParams(
            collective_id=0, has_side_effects=True, vmem_limit_bytes=48 * 2**20
        ),
    )(by_residue(queries), by_residue(keys), by_residue(values), w_out)
    mixed = mixed.reshape(DILATION_TWO, RATIO, piece, columns)
    return jnp.transpose(mixed, (2, 1, 0, 3)).reshape(tokens, columns)


def solution(mesh):
    in_specs = (P("sp", "tp", None), P("sp", "tp", None), P("sp", "tp", None), P(None, "tp"))
    out_specs = P("sp", "tp")
    return jax.shard_map(local, mesh=mesh, in_specs=in_specs, out_specs=out_specs, check_vma=False)
```

```python
import functools
import math

import jax
import jax.numpy as jnp
from jax import lax
from jax.experimental import pallas as pl
from jax.experimental.pallas import tpu as pltpu
from jax.sharding import PartitionSpec as P

W1 = 128
WINDOW_TWO = 512
DILATION_TWO = 4
WINDOW_THREE = 2048
DILATION_THREE = 16
MESH = pl.DeviceIdType.MESH
RATIO = DILATION_THREE // DILATION_TWO
CHUNKS = DILATION_TWO
ROWS_ONE = 16
ROWS_TWO = WINDOW_TWO // DILATION_THREE


def attend(blocks, scale):
    scores = [
        lax.dot_general(q, k, (((1,), (1,)), ((), ())), preferred_element_type=jnp.float32)
        for q, k, _, _ in blocks
    ]
    scores = [x * scale + bias for x, (_, _, _, bias) in zip(scores, blocks)]
    tops = [jnp.max(x, axis=-1, keepdims=True) for x in scores]
    numerators = [jnp.exp2(x - top) for x, top in zip(scores, tops)]
    sums = [
        jnp.dot(
            x.astype(v.dtype), jnp.concatenate([v, jnp.ones_like(v)], axis=1), preferred_element_type=jnp.float32
        )
        for x, (_, _, v, _) in zip(numerators, blocks)
    ]
    dim = blocks[0][2].shape[-1]
    return [(x[:, :dim], jnp.broadcast_to(top, x[:, :dim].shape), x[:, dim:]) for x, top in zip(sums, tops)]


def bias_of(shape, place_q, place_k, first_own, window, has_prev):
    query_place, _ = place_q(lax.broadcasted_iota(jnp.int32, shape, 0))
    key_place, key_row = place_k(lax.broadcasted_iota(jnp.int32, shape, 1))
    distance = query_place - key_place
    allowed = (distance >= 0) & (distance <= window)
    general = jnp.where(allowed, 0.0, -jnp.inf).astype(jnp.float32)
    gate = jnp.where(has_prev, 0, first_own)
    first = jnp.where(allowed & (key_row >= gate), 0.0, -jnp.inf).astype(jnp.float32)
    return general, first


def kernel(
    group, q_ref, k_ref, v_ref, w_ref, o_ref,
    qb, kb, vb, acc, mx, sm, ob, ab, bias1, bias1f, bias2, bias2f, bias3,
    in_send, in_recv, z_send, z_recv, zl_send, zl_recv, o_send, o_recv, d_send, d_recv,
):
    res, dim = DILATION_THREE, q_ref.shape[-1]
    piece = q_ref.shape[2]
    rows = group * piece
    sp, tp = lax.axis_index("sp"), lax.axis_index("tp")
    n_sp, n_tp = lax.axis_size("sp"), lax.axis_size("tp")
    mine = lax.rem(sp, group)
    base = sp - mine
    has_prev = sp >= group
    has_next = sp + group < n_sp
    partner = n_tp - 1 - tp
    scale = math.log2(math.e) / math.sqrt(dim)

    barrier = pltpu.get_barrier_semaphore()
    for d in range(1, group):
        pl.semaphore_signal(
            barrier, inc=1, device_id={"sp": base + lax.rem(mine + d, group)}, device_id_type=MESH
        )
    pl.semaphore_signal(barrier, inc=1, device_id={"tp": partner}, device_id_type=MESH)

    @pl.when(has_prev)
    def _():
        pl.semaphore_signal(barrier, inc=1, device_id={"sp": sp - group}, device_id_type=MESH)

    @pl.when(has_next)
    def _():
        pl.semaphore_signal(barrier, inc=1, device_id={"sp": sp + group}, device_id_type=MESH)

    pl.semaphore_wait(barrier, group + jnp.where(has_prev, 1, 0) + jnp.where(has_next, 1, 0))

    def span(start):
        return pl.ds(pl.multiple_of(start, piece), piece)

    tensors = ((k_ref, kb, rows), (v_ref, vb, rows), (q_ref, qb, 0))

    def member(d):
        other, bit = mine, 1
        while bit <= d:
            if d & bit:
                other = other + bit * (1 - 2 * lax.rem(mine // bit, 2))
            bit *= 2
        return other

    def exchange(which, d):
        source, buffer, offset = tensors[which]
        other = member(d)
        return pltpu.make_async_remote_copy(
            src_ref=source.at[other],
            dst_ref=buffer.at[:, span(offset + piece * mine), :],
            send_sem=in_send.at[which, d],
            recv_sem=in_recv.at[which, d],
            device_id={"sp": base + other},
            device_id_type=MESH,
        )

    def arrival(which, d):
        source, buffer, offset = tensors[which]
        return pltpu.make_async_remote_copy(
            src_ref=source.at[0],
            dst_ref=buffer.at[:, span(offset + piece * member(d)), :],
            send_sem=in_send.at[which, d],
            recv_sem=in_recv.at[which, d],
            device_id={"sp": sp},
            device_id_type=MESH,
        )

    low = piece - ROWS_ONE

    def onward_rows(which, k):
        source, buffer, _ = tensors[which]
        start = piece * member(k)
        if k == 0:
            src, dst = source.at[mine], buffer.at[:, span(start), :]
        elif k in whole:
            src, dst = buffer.at[:, span(rows + start), :], buffer.at[:, span(start), :]
        else:
            ends = [pl.ds(pl.multiple_of(x + start + low, ROWS_ONE), ROWS_ONE) for x in (rows, 0)]
            src, dst = (buffer.at[:, x, :] for x in ends)
        return pltpu.make_async_remote_copy(
            src_ref=src,
            dst_ref=dst,
            send_sem=z_send.at[which, k],
            recv_sem=z_recv.at[which, k],
            device_id={"sp": sp + group},
            device_id_type=MESH,
        )

    def onward_chunk(which, k, s):
        _, buffer, _ = tensors[which]
        start = piece * member(k)
        part = pl.ds(s * RATIO, RATIO)
        return pltpu.make_async_remote_copy(
            src_ref=buffer.at[part, pl.ds(pl.multiple_of(rows + start, ROWS_ONE), low), :],
            dst_ref=buffer.at[part, pl.ds(pl.multiple_of(start, ROWS_ONE), low), :],
            send_sem=zl_send.at[which, k, s],
            recv_sem=zl_recv.at[which, k, s],
            device_id={"sp": sp + group},
            device_id_type=MESH,
        )

    whole = range(group // 2)
    split = range(group // 2, group)

    @pl.when(has_next)
    def _():
        for which in (0, 1):
            onward_rows(which, 0).start()

    near = [d for d in range(1, group) if d & (d - 1) == 0]
    far = [d for d in range(1, group) if d & (d - 1)]
    for tensors_now in ((0, 1), (2,)):
        for members in (near, far):
            for which in tensors_now:
                for d in members:
                    exchange(which, d).start()

    for source, buffer, offset in tensors:
        buffer[:, span(offset + piece * mine), :] = source[mine]

    @pl.when(jnp.logical_not(has_prev))
    def _():
        kb[:, :rows, :] = jnp.zeros((res, rows, dim), kb.dtype)
        vb[:, :rows, :] = jnp.zeros((res, rows, dim), vb.dtype)

    def place_one(per):
        def place(i):
            store, row = i // per, i % per
            residue = (store % RATIO) * DILATION_TWO + store // RATIO
            return row * res + residue, row
        return place

    def place_two(per):
        def place(i):
            j, row = i // per, i % per
            return row * RATIO + j, row
        return place

    def shifted(place, by):
        def moved(i):
            at, row = place(i)
            return at + by, row
        return moved

    bias1[...], bias1f[...] = bias_of(
        bias1.shape, shifted(place_one(ROWS_ONE), ROWS_ONE * res), place_one(2 * ROWS_ONE), ROWS_ONE, W1, has_prev
    )
    bias2[...], bias2f[...] = bias_of(
        bias2.shape, shifted(place_two(ROWS_TWO), ROWS_TWO * RATIO), place_two(2 * ROWS_TWO), ROWS_TWO,
        WINDOW_TWO // DILATION_TWO, has_prev,
    )
    _, bias3[...] = bias_of(
        bias3.shape, lambda i: (i + rows, i), lambda i: (i, i), rows, WINDOW_THREE // DILATION_THREE, has_prev
    )

    for k in range(1, group):
        for which in (0, 1):
            arrival(which, k).wait_recv()

        @pl.when(has_next)
        def _():
            for which in (0, 1):
                onward_rows(which, k).start()

    @pl.when(has_next)
    def _():
        for s in range(CHUNKS):
            for k in split:
                for which in (0, 1):
                    onward_chunk(which, k, s).start()

    def branch_one(blocks, bias):
        spans = [
            (
                pl.ds(pl.multiple_of(b * ROWS_ONE, ROWS_ONE), ROWS_ONE),
                pl.ds(pl.multiple_of(rows + (b - 1) * ROWS_ONE, ROWS_ONE), 2 * ROWS_ONE),
            )
            for b in blocks
        ]
        found = attend(
            [
                tuple(x[:, at, :].reshape(-1, dim) for x, at in ((qb, own), (kb, near), (vb, near))) + (bias[...],)
                for own, near in spans
            ],
            scale,
        )
        for (own, _), (weighted, top, total) in zip(spans, found):
            acc[:, own, :] = weighted.reshape(res, ROWS_ONE, dim)
            mx[:, own, :] = top.reshape(res, ROWS_ONE, dim)
            sm[:, own, :] = total.reshape(res, ROWS_ONE, dim)

    def merge(at, weighted, top, total):
        old_top = mx[at].reshape(-1, dim)
        new_top = jnp.maximum(old_top, top)
        old_part, part = jnp.exp2(old_top - new_top), jnp.exp2(top - new_top)
        return (
            acc[at].reshape(-1, dim) * old_part + weighted * part,
            new_top,
            sm[at].reshape(-1, dim) * old_part + total * part,
        )

    def branch_two(blocks, bias):
        spans = [
            (
                pl.ds(s * RATIO, RATIO),
                pl.ds(b * ROWS_TWO, ROWS_TWO),
                pl.ds(rows + (b - 1) * ROWS_TWO, 2 * ROWS_TWO),
            )
            for s, b in blocks
        ]
        found = attend(
            [
                tuple(x[part, at, :].reshape(-1, dim) for x, at in ((qb, own), (kb, near), (vb, near))) + (bias[...],)
                for part, own, near in spans
            ],
            scale,
        )
        merged = [merge((part, own, slice(None)), *one) for (part, own, _), one in zip(spans, found)]
        for (part, own, _), (weighted, top, total) in zip(spans, merged):
            acc[part, own, :] = weighted.reshape(RATIO, ROWS_TWO, dim)
            mx[part, own, :] = top.reshape(RATIO, ROWS_TWO, dim)
            sm[part, own, :] = total.reshape(RATIO, ROWS_TWO, dim)

    def some(items, count):
        return [items[i : i + count] for i in range(0, len(items), count)]

    steps = piece // ROWS_ONE
    for d in [0] + near + far:
        if d:
            arrival(2, d).wait_recv()
        for inner in range(1, steps):
            branch_one([member(d) * steps + inner], bias1)
    for b in range(steps, rows // ROWS_ONE, steps):
        branch_one([b], bias1)
    for blocks in some([(s, b) for s in range(CHUNKS) for b in range(1, rows // ROWS_TWO)], 2):
        branch_two(blocks, bias2)

    @pl.when(has_prev)
    def _():
        for k in range(group):
            for which in (0, 1):
                onward_rows(which, k).wait_recv()

    branch_one([0], bias1f)

    head = tp * group + mine

    def lanes(index):
        return pl.ds(pl.multiple_of(index * dim, dim), dim)

    def give(s, d):
        part = pl.ds(s * RATIO, RATIO)
        other = member(d)
        return pltpu.make_async_remote_copy(
            src_ref=ob.at[part, span(piece * other), :],
            dst_ref=ab.at[part, :, lanes(head)],
            send_sem=o_send.at[s, d],
            recv_sem=o_recv.at[s, d],
            device_id={"sp": base + other},
            device_id_type=MESH,
        )

    def taken(s, d):
        part = pl.ds(s * RATIO, RATIO)
        return pltpu.make_async_remote_copy(
            src_ref=ob.at[part, span(0), :],
            dst_ref=ab.at[part, :, lanes(tp * group + member(d))],
            send_sem=o_send.at[s, d],
            recv_sem=o_recv.at[s, d],
            device_id={"sp": sp},
            device_id_type=MESH,
        )

    def swap(s, d):
        part = pl.ds(s * RATIO, RATIO)
        slot = ab.at[part, :, lanes(tp * group + member(d))]
        return pltpu.make_async_remote_copy(
            src_ref=ob.at[part, span(piece * mine), :] if d == 0 else slot,
            dst_ref=slot,
            send_sem=d_send.at[s, d],
            recv_sem=d_recv.at[s, d],
            device_id={"tp": partner},
            device_id_type=MESH,
        )

    def swapped(s, d):
        part = pl.ds(s * RATIO, RATIO)
        return pltpu.make_async_remote_copy(
            src_ref=ob.at[part, span(0), :],
            dst_ref=ab.at[part, :, lanes(partner * group + member(d))],
            send_sem=d_send.at[s, d],
            recv_sem=d_recv.at[s, d],
            device_id={"tp": partner},
            device_id_type=MESH,
        )

    def hand_over(s):
        for d in range(1, group):
            taken(s, d).wait_recv()
            swap(s, d).start()

    def project(s):
        part = pl.ds(s * RATIO, RATIO)
        for d in range(group):
            swapped(s, d).wait_recv()
        attended = ab[part].reshape(RATIO * piece, -1)
        mixed = jnp.dot(attended, w_ref[...], preferred_element_type=jnp.float32)
        o_ref[part] = mixed.astype(o_ref.dtype).reshape(RATIO, piece, -1)

    for s in range(CHUNKS):
        part = pl.ds(s * RATIO, RATIO)

        @pl.when(has_prev)
        def _():
            for k in split:
                for which in (0, 1):
                    onward_chunk(which, k, s).wait_recv()

        branch_two([(s, 0)], bias2f)
        for stores in some(list(range(s * RATIO, (s + 1) * RATIO)), 2):
            found = attend([(qb[x], kb[x], vb[x], bias3[...]) for x in stores], scale)
            for x, one in zip(stores, found):
                weighted, _, total = merge((x,), *one)
                ob[x] = (weighted / total).astype(ob.dtype)
        for d in far + near:
            give(s, d).start()
        swap(s, 0).start()
        ab[part, :, lanes(head)] = ob[part, span(piece * mine), :]
        if s >= 2:
            hand_over(s - 2)
    for s in range(CHUNKS - 2, CHUNKS):
        hand_over(s)
        project(s - 2)
    for s in range(CHUNKS - 2, CHUNKS):
        project(s)

    for which in (0, 1, 2):
        for d in range(1, group):
            exchange(which, d).wait_send()

    @pl.when(has_next)
    def _():
        for which in (0, 1):
            for k in range(group):
                onward_rows(which, k).wait_send()
            for k in split:
                for s in range(CHUNKS):
                    onward_chunk(which, k, s).wait_send()

    for s in range(CHUNKS):
        for d in range(1, group):
            give(s, d).wait_send()
        for d in range(group):
            swap(s, d).wait_send()


def local(queries, keys, values, w_out):
    tokens, group, dim = queries.shape
    features, columns = w_out.shape
    res = DILATION_THREE
    piece = tokens // res
    rows = group * piece
    assert group & (group - 1) == 0 and piece > ROWS_ONE
    assert group * tokens == WINDOW_THREE and lax.axis_size("sp") % group == 0 and lax.axis_size("tp") == 2

    def by_residue(x):
        x = x.reshape(piece, RATIO, DILATION_TWO, group, dim)
        return jnp.transpose(x, (3, 2, 1, 0, 4)).reshape(group, res, piece, dim)

    low, full = jnp.bfloat16, jnp.float32
    dma = pltpu.SemaphoreType.DMA
    vmem = pl.BlockSpec(memory_space=pltpu.VMEM)
    mixed = pl.pallas_call(
        functools.partial(kernel, group),
        out_shape=jax.ShapeDtypeStruct((res, piece, columns), low),
        in_specs=[vmem] * 4,
        out_specs=vmem,
        scratch_shapes=[
            pltpu.VMEM((res, rows, dim), low),
            pltpu.VMEM((res, 2 * rows, dim), low),
            pltpu.VMEM((res, 2 * rows, dim), low),
            pltpu.VMEM((res, rows, dim), full),
            pltpu.VMEM((res, rows, dim), full),
            pltpu.VMEM((res, rows, dim), full),
            pltpu.VMEM((res, rows, dim), low),
            pltpu.VMEM((res, piece, features), low),
            pltpu.VMEM((res * ROWS_ONE, 2 * res * ROWS_ONE), full),
            pltpu.VMEM((res * ROWS_ONE, 2 * res * ROWS_ONE), full),
            pltpu.VMEM((RATIO * ROWS_TWO, 2 * RATIO * ROWS_TWO), full),
            pltpu.VMEM((RATIO * ROWS_TWO, 2 * RATIO * ROWS_TWO), full),
            pltpu.VMEM((rows, 2 * rows), full),
            dma((3, group)), dma((3, group)),
            dma((2, group)), dma((2, group)),
            dma((2, group, CHUNKS)), dma((2, group, CHUNKS)),
            dma((CHUNKS, group)), dma((CHUNKS, group)),
            dma((CHUNKS, group)), dma((CHUNKS, group)),
        ],
        compiler_params=pltpu.CompilerParams(
            collective_id=0, has_side_effects=True, vmem_limit_bytes=48 * 2**20
        ),
    )(by_residue(queries), by_residue(keys), by_residue(values), w_out)
    mixed = mixed.reshape(DILATION_TWO, RATIO, piece, columns)
    return jnp.transpose(mixed, (2, 1, 0, 3)).reshape(tokens, columns)


def solution(mesh):
    in_specs = (P("sp", "tp", None), P("sp", "tp", None), P("sp", "tp", None), P(None, "tp"))
    out_specs = P("sp", "tp")
    return jax.shard_map(local, mesh=mesh, in_specs=in_specs, out_specs=out_specs, check_vma=False)
```
